32 devices in a mesh: kv: 8 (over z, y), tp: 4 (over x, core).
Axes of the slice: x: 2, y: 2, z: 4, core: 2. Of those that a mesh axis runs over, the one named last changes fastest.
Arguments:
- tokens: bfloat16 [32, 4096], P(None, ('kv', 'tp')), may hold values from -36 to 36
- first_gain: float32 [4096], P('kv'), may hold values from 0.1 to 1.9
- first_gate: bfloat16 [4096, 11264], P('kv', 'tp'), may hold values from -0.09375 to 0.09375
- first_up: bfloat16 [4096, 11264], P('kv', 'tp'), may hold values from -0.09375 to 0.09375
- first_down: bfloat16 [11264, 4096], P('tp', 'kv'), may hold values from -0.0546875 to 0.0546875
- mix_gain: float32 [4096], P('kv'), may hold values from 0.1 to 1.9
- w_query: bfloat16 [4096, 2048], P('kv', 'tp'), may hold values from -0.09375 to 0.09375
- key_cache: bfloat16 [32, 8192, 1024], P(None, 'kv', 'tp'), may hold values from -100 to 100
- value_cache: bfloat16 [32, 8192, 1024], P(None, 'kv', 'tp'), may hold values from -6 to 6
- map_weight: float32 [32], P('tp'), may hold values from 0.3 to 0.8
- head_gain: float32 [64], replicated, may hold values from 0.1 to 1.9
- w_out: bfloat16 [2048, 4096], P('tp', 'kv'), may hold values from -0.125 to 0.125
- second_gain: float32 [4096], P('kv'), may hold values from 0.1 to 1.9
- second_gate: bfloat16 [4096, 11264], P('kv', 'tp'), may hold values from -0.09375 to 0.09375
- second_up: bfloat16 [4096, 11264], P('kv', 'tp'), may hold values from -0.09375 to 0.09375
- second_down: bfloat16 [11264, 4096], P('tp', 'kv'), may hold values from -0.0546875 to 0.0546875
Outputs:
- mixed: bfloat16 [32, 4096], P(None, ('kv', 'tp'))
The draws below stay inside these ranges and needn't reach their ends.
All inputs are finite; a program needn't handle non-finite values.
Results may differ from the reference program's by a relative error of at most 0.0158.
Values may be sent and summed in bfloat16 or wider, within the bound.
A program may use at most 128 MiB of HBM per device.

```python
import math
import jax
import jax.numpy as jnp
from jax import lax

D = 4096
FF = 11264
HEADS = 32
KV_HEADS = 16
HEAD = 64
HALF = 32
BATCH = 32
LENGTH = 8192
DKV = 512


def draw_tokens(key, part):
    columns = jnp.arange(D, dtype=jnp.float32)
    inner = jnp.arange(D, dtype=jnp.int32) % DKV
    col_scale = 3.0 ** (columns / D - 0.5) * 3.0 ** (inner.astype(jnp.float32) / DKV - 0.5)
    row_scale = jnp.exp(jax.random.uniform(jax.random.fold_in(key, 1), (BATCH, 1), jnp.float32, math.log(0.3), math.log(3.0)))
    entries = jnp.clip(jax.random.normal(jax.random.fold_in(key, 2), (BATCH, D), jnp.float32), -4.0, 4.0)
    return (entries * row_scale * col_scale[None, :]).astype(jnp.bfloat16)


def draw_key_cache(key, part):
    width = KV_HEADS * HEAD
    base = jnp.clip(jax.random.normal(jax.random.fold_in(key, 11), (BATCH, LENGTH, width), jnp.float32), -6.0, 6.0) * 1.75
    return base.astype(jnp.bfloat16)


def shard_levels(key, dims, pieces, smallest, largest):
    level, own = 1.0, jax.random.fold_in(key, 6)
    for dim, blocks in pieces:
        draws = jnp.exp(jax.random.uniform(jax.random.fold_in(own, dim), (blocks,), jnp.float32, smallest / len(pieces), largest / len(pieces)))
        level = level * jnp.repeat(draws, dims[dim] // blocks).reshape([-1 if axis == dim else 1 for axis in range(len(dims))])
    return level


def scatter_about(key, extent, deviation, most, shards=(), kind=jnp.bfloat16):
    array = deviation * jax.random.normal(key, extent, jnp.float32)
    if shards:
        array = array * shard_levels(key, extent, shards, -0.22, 0.18)
    return jnp.clip(array, -most, most).astype(kind)


def setup_inputs(seed: int = 0) -> dict:
    streams_of = jax.random.split(jax.random.key(seed), 17)
    tokens = draw_tokens(jax.random.fold_in(streams_of[16], 71), 0)
    first_gain = jnp.clip(1.0 + 0.18 * jax.random.normal(streams_of[1], (D,), jnp.float32), 0.1, 1.9)
    first_gate = scatter_about(streams_of[2], (D, FF), D ** -0.5, 0.09375, ((0, 8), (1, 4)))
    first_up = scatter_about(streams_of[3], (D, FF), D ** -0.5, 0.09375, ((0, 8), (1, 4)))
    first_down = scatter_about(streams_of[4], (FF, D), FF ** -0.5, 0.0546875, ((0, 4), (1, 8)))
    mix_gain = jnp.clip(1.0 + 0.18 * jax.random.normal(streams_of[5], (D,), jnp.float32), 0.1, 1.9)
    w_query = scatter_about(streams_of[6], (D, HEADS * HEAD), D ** -0.5, 0.09375, ((0, 8), (1, 4)))
    key_cache = draw_key_cache(jax.random.fold_in(streams_of[16], 71), 0)
    value_cache = scatter_about(streams_of[8], (BATCH, LENGTH, KV_HEADS * HEAD), 1.0, 6.0, ((1, 8), (2, 4)))
    map_weight = jnp.clip(0.3 + 0.5 * jax.random.uniform(streams_of[9], (HEADS,), jnp.float32) ** shard_levels(streams_of[9], (HEADS,), ((0, 4),), -0.2, 0.2), 0.3, 0.8)
    head_gain = jnp.clip(1.0 + 0.18 * jax.random.normal(streams_of[10], (HEAD,), jnp.float32), 0.1, 1.9)
    w_out = scatter_about(streams_of[11], (HEADS * HEAD, D), (HEADS * HEAD) ** -0.5, 0.125, ((0, 4), (1, 8)))
    second_gain = jnp.clip(1.0 + 0.18 * jax.random.normal(streams_of[12], (D,), jnp.float32), 0.1, 1.9)
    second_gate = scatter_about(streams_of[13], (D, FF), D ** -0.5, 0.09375, ((0, 8), (1, 4)))
    second_up = scatter_about(streams_of[14], (D, FF), D ** -0.5, 0.09375, ((0, 8), (1, 4)))
    second_down = scatter_about(streams_of[15], (FF, D), FF ** -0.5, 0.0546875, ((0, 4), (1, 8)))
    return dict(tokens=tokens, first_gain=first_gain, first_gate=first_gate, first_up=first_up, first_down=first_down, mix_gain=mix_gain, w_query=w_query, key_cache=key_cache, value_cache=value_cache, map_weight=map_weight, head_gain=head_gain, w_out=w_out, second_gain=second_gain, second_gate=second_gate, second_up=second_up, second_down=second_down)


EPS = 1e-06
HEAD_SCALE = 0.8

def channel_mixer(residual, gain, w_gate, w_up, w_down):
    factor = lax.rsqrt(lax.optimization_barrier(jnp.mean(residual * residual, axis=1, keepdims=True)) + EPS)
    scaled = (residual * gain).astype(jnp.bfloat16)
    gate_sum = factor * jnp.dot(scaled, w_gate, preferred_element_type=jnp.float32)
    up_sum = factor * jnp.dot(scaled, w_up, preferred_element_type=jnp.float32)
    active = (jax.nn.silu(gate_sum) * up_sum).astype(jnp.bfloat16)
    return jnp.dot(active, w_down, preferred_element_type=jnp.float32)

def attention_mix(residual, mix_gain, w_query, key_cache, value_cache, map_weight, head_gain, w_out):
    factor = lax.rsqrt(lax.optimization_barrier(jnp.mean(residual * residual, axis=1, keepdims=True)) + EPS)
    scaled = (residual * mix_gain).astype(jnp.bfloat16)
    queries = (factor * jnp.dot(scaled, w_query, preferred_element_type=jnp.float32)).astype(jnp.bfloat16)
    group = HEADS // KV_HEADS

    def one_row(items):
        row_query, row_keys, row_values = items
        query_full = row_query.astype(jnp.float32).reshape(KV_HEADS, group, HEAD)
        keys_full = row_keys.astype(jnp.float32).reshape(-1, KV_HEADS, HEAD)
        values_full = row_values.astype(jnp.float32).reshape(-1, KV_HEADS, HEAD)

        def one_map(first_col, last_col):
            scores = jnp.einsum('kgd,pkd->kgp', query_full[..., first_col:last_col], keys_full[..., first_col:last_col]) / math.sqrt(last_col - first_col)
            row_peak = lax.optimization_barrier(jnp.max(scores, axis=2, keepdims=True))
            exp_terms = jnp.exp(scores - row_peak)
            weights_sum = lax.optimization_barrier(jnp.sum(exp_terms, axis=2))
            rounded = lax.optimization_barrier(exp_terms.astype(jnp.bfloat16)).astype(jnp.float32)
            return jnp.einsum('kgp,pkd->kgd', rounded, values_full) / weights_sum[..., None]
        return (one_map(0, HALF), one_map(HALF, HEAD))
    out_one, out_two = lax.map(one_row, (queries, key_cache, value_cache))
    combined = out_one - map_weight.reshape(KV_HEADS, group)[..., None] * out_two
    normed = combined * lax.rsqrt(lax.optimization_barrier(jnp.mean(combined * combined, axis=3, keepdims=True)) + EPS) * head_gain * HEAD_SCALE
    normed = normed.astype(jnp.bfloat16).reshape(BATCH, HEADS * HEAD)
    return jnp.dot(normed, w_out, preferred_element_type=jnp.float32)

def reference(tokens, first_gain, first_gate, first_up, first_down, mix_gain, w_query, key_cache, value_cache, map_weight, head_gain, w_out, second_gain, second_gate, second_up, second_down):
    residual = tokens.astype(jnp.float32)
    residual = residual + 0.5 * channel_mixer(residual, first_gain, first_gate, first_up, first_down)
    residual = residual + attention_mix(residual, mix_gain, w_query, key_cache, value_cache, map_weight, head_gain, w_out)
    residual = residual + 0.5 * channel_mixer(residual, second_gain, second_gate, second_up, second_down)
    return residual.astype(jnp.bfloat16)
```

```python
import functools
import math

import jax
import jax.numpy as jnp
from jax import lax
from jax.experimental import pallas as pl
from jax.experimental.pallas import tpu as pltpu
from jax.sharding import PartitionSpec as P

HEAD = 64
MAPS = 2
LANES = 128
TILE = 8
EPS = 1e-06
HEAD_SCALE = 0.8
F32 = jnp.float32
BF16 = jnp.bfloat16
MESH = pl.DeviceIdType.MESH
VMEM_LIMIT = 60 * 1024 * 1024


def greet(axes):
    barrier = pltpu.get_barrier_semaphore()
    total = 0
    for axis, n in axes:
        me = lax.axis_index(axis)
        for k in range(1, n):
            pl.semaphore_signal(
                barrier, inc=1, device_id={axis: lax.rem(me + k, n)}, device_id_type=MESH
            )
        total += n - 1
    pl.semaphore_wait(barrier, total)


def exchange(axis, n, source, target, sems):
    me = lax.axis_index(axis)
    copies = []
    for k in range(1, n):
        dest = lax.rem(me + k, n)
        copy = pltpu.make_async_remote_copy(
            src_ref=source(dest),
            dst_ref=target(k - 1),
            send_sem=sems.at[0, k - 1],
            recv_sem=sems.at[1, k - 1],
            device_id={axis: dest},
            device_id_type=MESH,
        )
        copy.start()
        copies.append(copy)
    return copies


def total_of(copies, own, recv):
    total = own
    for k, copy in enumerate(copies):
        copy.wait()
        total = total + recv[k].astype(F32)
    return total


def squares_tile(h):
    s = jnp.sum(h * h, axis=1, keepdims=True)
    high = s.astype(BF16).astype(F32)
    lane = lax.broadcasted_iota(jnp.int32, (h.shape[0], LANES), 1)
    return jnp.where(lane < LANES // 2, high, s - high).astype(BF16)


def row_factor(tile, width):
    s = tile[:, :1] + tile[:, LANES // 2 : LANES // 2 + 1]
    return lax.rsqrt(s / width + EPS)


def chunk_width(hidden, n):
    return -(-hidden // (LANES * n)) * LANES


def dot(a, b):
    return jnp.dot(a, b, preferred_element_type=F32)


def feed_forward(n_kv, h, gain, w_gate, w_up, w_down, loads, scratch):
    send, recv, act_own, act_all, rs_sems, ag_sems = scratch
    me = lax.axis_index("kv")
    hidden = w_gate.shape[1]
    cw = chunk_width(hidden, n_kv)
    rows = h.shape[0]
    tile = squares_tile(h)
    scaled = (h * gain).astype(BF16)
    loads[0].wait()
    loads[1].wait()
    for j in range(n_kv):
        low = min(j * cw, hidden)
        w = min(cw, hidden - low)
        for base, weight in ((0, w_gate), (cw, w_up)):
            if w > 0:
                send[j, :, base : base + w] = dot(scaled, weight[:, low : low + w]).astype(BF16)
            if w < cw:
                send[j, :, base + w : base + cw] = jnp.zeros((rows, cw - w), BF16)
        send[j, :, 2 * cw :] = tile
    copies = exchange("kv", n_kv, lambda d: send.at[d], lambda k: recv.at[k], rs_sems)
    total = total_of(copies, send[me].astype(F32), recv)
    factor = row_factor(total[:, 2 * cw :], h.shape[1] * n_kv)
    gate = total[:, :cw] * factor
    up = total[:, cw : 2 * cw] * factor
    act = (gate / (1.0 + jnp.exp(-gate)) * up).astype(BF16)
    act_own[...] = act
    mine = pl.ds(pl.multiple_of(me * cw, LANES), cw)
    act_all[:, mine] = act
    copies = exchange("kv", n_kv, lambda d: act_own, lambda k: act_all.at[:, mine], ag_sems)
    for copy in copies:
        copy.wait()
    loads[2].wait()
    return dot(act_all[:, :hidden], w_down[...])


def sum_over_tp(n_tp, part, send, recv, sems):
    send[...] = part.astype(BF16)
    copies = exchange("tp", n_tp, lambda d: send, lambda k: recv.at[k], sems)
    return total_of(copies, send[...].astype(F32), recv)


def start_loads(pairs, sems):
    loads = [pltpu.make_async_copy(a, b, sems.at[i]) for i, (a, b) in enumerate(pairs)]
    for load in loads:
        load.start()
    return loads


def first_kernel(
    n_kv, n_tp, tokens, gain, mix_gain, gate_any, up_any, down_any, query_any, h_out, q_out,
    w_gate, w_up, w_down, w_query, tok_all, rs_send, rs_recv, act_own, act_all,
    tp_send, tp_recv, q_send, q_recv, load_sems, tok_sems, rs_sems, ag_sems, tp_sems, q_sems,
):
    loads = start_loads(
        ((gate_any, w_gate), (up_any, w_up), (down_any, w_down), (query_any, w_query)), load_sems
    )
    greet((("kv", n_kv), ("tp", n_tp)))
    tp = lax.axis_index("tp")
    tok_all[tp] = tokens[...]
    copies = exchange("tp", n_tp, lambda d: tokens, lambda k: tok_all.at[tp], tok_sems)
    for copy in copies:
        copy.wait()
    h = jnp.concatenate([tok_all[j].astype(F32) for j in range(n_tp)], axis=1)
    part = feed_forward(
        n_kv, h, gain[...], w_gate, w_up, w_down, loads,
        (rs_send, rs_recv, act_own, act_all, rs_sems, ag_sems),
    )
    h = h + 0.5 * sum_over_tp(n_tp, part, tp_send, tp_recv, tp_sems)
    h_out[...] = h
    loads[3].wait()
    columns = w_query.shape[1]
    q_send[:, :columns] = dot((h * mix_gain[...]).astype(BF16), w_query[...]).astype(BF16)
    q_send[:, columns:] = squares_tile(h)
    copies = exchange("kv", n_kv, lambda d: q_send, lambda k: q_recv.at[k], q_sems)
    total = total_of(copies, q_send[...].astype(F32), q_recv)
    factor = row_factor(total[:, columns:], h.shape[1] * n_kv)
    q_out[...] = (total[:, :columns] * factor).astype(BF16)


def attention_kernel(kv_local, per_tile, scale, q_ref, k_ref, v_ref, o_ref, lse_ref):
    wide = lax.broadcasted_iota(jnp.int32, (TILE, kv_local * HEAD), 1) // HEAD
    lane = lax.broadcasted_iota(jnp.int32, (TILE, LANES), 1)
    part_rows = TILE // per_tile
    wide_row = lax.broadcasted_iota(jnp.int32, (TILE, kv_local * HEAD), 0) // part_rows
    lane_row = lax.broadcasted_iota(jnp.int32, (TILE, LANES), 0) // part_rows
    tiles_o, tiles_lse = [], []
    for first in range(0, q_ref.shape[0], per_tile):
        tile_o = jnp.zeros((TILE, kv_local * HEAD), F32)
        tile_lse = jnp.zeros((TILE, LANES), F32)
        for i in range(per_tile):
            b = first + i
            s = scale * lax.dot_general(
                q_ref[b], k_ref[b], (((1,), (1,)), ((), ())), preferred_element_type=F32
            )
            peak = jnp.max(s, axis=1, keepdims=True)
            e = jnp.exp(s - peak)
            l = jnp.sum(e, axis=1, keepdims=True)
            o = dot(e.astype(BF16), v_ref[b]) / l
            lse = peak + jnp.log(l)
            for k in range(kv_local):
                rows = slice(k * TILE, (k + 1) * TILE)
                tile_o = jnp.where((wide == k) & (wide_row == i), o[rows], tile_o)
                tile_lse = jnp.where((lane == k) & (lane_row == i), lse[rows], tile_lse)
        tiles_o.append(tile_o)
        tiles_lse.append(tile_lse)
    o_ref[0] = jnp.concatenate(tiles_o, axis=0).astype(BF16)
    lse_ref[0] = jnp.concatenate(tiles_lse, axis=0)


def second_kernel(
    n_kv, n_tp, kv_local, group, h_in, o_part, lse_part, map_weight, head_gain, gain,
    out_any, gate_any, up_any, down_any, mixed,
    w_out, w_gate, w_up, w_down, o_recv, lse_recv, head_own, head_all, rs_send, rs_recv,
    act_own, act_all, tp_send, tp_recv, fin_send, fin_recv,
    load_sems, o_sems, lse_sems, head_sems, rs_sems, ag_sems, tp_sems, fin_sems,
):
    loads = start_loads(
        ((out_any, w_out), (gate_any, w_gate), (up_any, w_up), (down_any, w_down)), load_sems
    )
    greet((("kv", n_kv), ("tp", n_tp)))
    me = lax.axis_index("kv")
    copies = exchange("kv", n_kv, lambda d: o_part.at[d], lambda k: o_recv.at[k], o_sems)
    copies += exchange("kv", n_kv, lambda d: lse_part.at[d], lambda k: lse_recv.at[k], lse_sems)
    for copy in copies:
        copy.wait()
    lses = [lse_part[me]] + [lse_recv[k] for k in range(n_kv - 1)]
    outs = [o_part[me].astype(F32)] + [o_recv[k].astype(F32) for k in range(n_kv - 1)]
    peak = functools.reduce(jnp.maximum, lses)
    weights = [jnp.exp(lse - peak) for lse in lses]
    scale = 1.0 / functools.reduce(jnp.add, weights)
    slab = outs[0].shape
    head_of = lax.broadcasted_iota(jnp.int32, slab, 1) // HEAD

    def widen(value):
        wide = jnp.zeros(slab, F32)
        for k in range(kv_local):
            wide = jnp.where(head_of == k, value[:, k : k + 1], wide)
        return wide

    merged = functools.reduce(
        jnp.add, [widen(weight * scale) * out for weight, out in zip(weights, outs)]
    )
    diff = merged - map_weight[...] * pltpu.roll(merged, slab[0] - group, 0)
    square = diff * diff
    mean = jnp.zeros(slab, F32)
    for k in range(kv_local):
        here = jnp.sum(jnp.where(head_of == k, square, 0.0), axis=1, keepdims=True) / HEAD
        mean = jnp.where(head_of == k, here, mean)
    head_own[...] = (diff * lax.rsqrt(mean + EPS) * head_gain[...] * HEAD_SCALE).astype(BF16)
    head_all[me] = head_own[...]
    copies = exchange("kv", n_kv, lambda d: head_own, lambda k: head_all.at[me], head_sems)
    for copy in copies:
        copy.wait()
    heads = head_all[...].reshape(n_kv * slab[0], slab[1])
    loads[0].wait()
    batch = h_in.shape[0]
    pick_row = lax.broadcasted_iota(jnp.int32, (batch, heads.shape[0]), 0)
    pick_col = lax.broadcasted_iota(jnp.int32, (batch, heads.shape[0]), 1)
    part = None
    for g in range(group):
        pick = jnp.where(pick_col == pick_row * (MAPS * group) + g, 1.0, 0.0).astype(BF16)
        picked = dot(pick, heads).astype(BF16)
        weight = jnp.concatenate(
            [w_out[(k * group + g) * HEAD : (k * group + g + 1) * HEAD, :] for k in range(kv_local)],
            axis=0,
        )
        term = dot(picked, weight)
        part = term if part is None else part + term
    h = h_in[...] + sum_over_tp(n_tp, part, tp_send, tp_recv, tp_sems)
    part = feed_forward(
        n_kv, h, gain[...], w_gate, w_up, w_down, loads[1:],
        (rs_send, rs_recv, act_own, act_all, rs_sems, ag_sems),
    )
    width = mixed.shape[1]
    tp = lax.axis_index("tp")
    mine = jnp.zeros((batch, width), F32)
    for j in range(n_tp):
        columns = slice(j * width, (j + 1) * width)
        fin_send[j] = part[:, columns].astype(BF16)
        mine = jnp.where(tp == j, h[:, columns], mine)
    copies = exchange("tp", n_tp, lambda d: fin_send.at[d], lambda k: fin_recv.at[k], fin_sems)
    total = total_of(copies, fin_send[tp].astype(F32), fin_recv)
    mixed[...] = (mine + 0.5 * total).astype(BF16)


def dma_sems(n):
    return pltpu.SemaphoreType.DMA((2, n - 1))


def on_device(
    n_kv, n_tp, tokens, first_gain, first_gate, first_up, first_down, mix_gain, w_query,
    key_cache, value_cache, map_weight, head_gain, w_out, second_gain, second_gate, second_up,
    second_down,
):
    batch = tokens.shape[0]
    depth, hidden = first_gate.shape
    length = key_cache.shape[1]
    columns = w_query.shape[1]
    kv_local = key_cache.shape[2] // HEAD
    group = columns // (kv_local * HEAD)
    cw = chunk_width(hidden, n_kv)
    vmem = pl.BlockSpec(memory_space=pltpu.VMEM)
    hbm = pl.BlockSpec(memory_space=pl.ANY)
    ffn_buffers = [
        pltpu.VMEM((n_kv, batch, 2 * cw + LANES), BF16),
        pltpu.VMEM((n_kv - 1, batch, 2 * cw + LANES), BF16),
        pltpu.VMEM((batch, cw), BF16),
        pltpu.VMEM((batch, n_kv * cw), BF16),
    ]
    tp_buffers = [pltpu.VMEM((batch, depth), BF16), pltpu.VMEM((n_tp - 1, batch, depth), BF16)]

    def params(number):
        return pltpu.CompilerParams(
            collective_id=number, has_side_effects=True, vmem_limit_bytes=VMEM_LIMIT
        )

    h1, queries = pl.pallas_call(
        functools.partial(first_kernel, n_kv, n_tp),
        out_shape=(
            jax.ShapeDtypeStruct((batch, depth), F32),
            jax.ShapeDtypeStruct((batch, columns), BF16),
        ),
        in_specs=[vmem] * 3 + [hbm] * 4,
        out_specs=(vmem, vmem),
        scratch_shapes=[
            pltpu.VMEM(first_gate.shape, BF16),
            pltpu.VMEM(first_up.shape, BF16),
            pltpu.VMEM(first_down.shape, BF16),
            pltpu.VMEM(w_query.shape, BF16),
            pltpu.VMEM((n_tp,) + tokens.shape, BF16),
            *ffn_buffers,
            *tp_buffers,
            pltpu.VMEM((batch, columns + LANES), BF16),
            pltpu.VMEM((n_kv - 1, batch, columns + LANES), BF16),
            pltpu.SemaphoreType.DMA((4,)),
            dma_sems(n_tp),
            dma_sems(n_kv),
            dma_sems(n_kv),
            dma_sems(n_tp),
            dma_sems(n_kv),
        ],
        compiler_params=params(1),
    )(
        tokens, first_gain.reshape(1, -1), mix_gain.reshape(1, -1),
        first_gate, first_up, first_down, w_query,
    )

    per_tile = TILE // (MAPS * group)
    q = queries.reshape(batch, kv_local, 1, group, HEAD)
    half = (jnp.arange(HEAD) // (HEAD // MAPS))[None, :] == jnp.arange(MAPS)[:, None]
    q = jnp.where(half[None, None, :, None, :], q, 0).reshape(batch, kv_local, 1, MAPS * group, 1, HEAD)
    place = (jnp.arange(batch) % per_tile)[:, None] == jnp.arange(per_tile)[None, :]
    own = jnp.arange(kv_local)[:, None] == jnp.arange(kv_local)[None, :]
    keep = place[:, None, :, None, None, None] & own[None, :, None, None, :, None]
    q = jnp.where(keep, q, 0).reshape(batch, kv_local * TILE, kv_local * HEAD)

    each = batch // n_kv
    slab_rows = each // per_tile * TILE
    o_part, lse_part = pl.pallas_call(
        functools.partial(attention_kernel, kv_local, per_tile, 1.0 / math.sqrt(HEAD // MAPS)),
        grid=(n_kv,),
        out_shape=(
            jax.ShapeDtypeStruct((n_kv, slab_rows, kv_local * HEAD), BF16),
            jax.ShapeDtypeStruct((n_kv, slab_rows, LANES), F32),
        ),
        in_specs=[
            pl.BlockSpec((each, kv_local * TILE, kv_local * HEAD), lambda i: (i, 0, 0)),
            pl.BlockSpec((each, length, kv_local * HEAD), lambda i: (i, 0, 0)),
            pl.BlockSpec((each, length, kv_local * HEAD), lambda i: (i, 0, 0)),
        ],
        out_specs=(
            pl.BlockSpec((1, slab_rows, kv_local * HEAD), lambda i: (i, 0, 0)),
            pl.BlockSpec((1, slab_rows, LANES), lambda i: (i, 0, 0)),
        ),
        compiler_params=pltpu.CompilerParams(vmem_limit_bytes=VMEM_LIMIT),
    )(q, key_cache, value_cache)

    weight = jnp.repeat(map_weight.reshape(kv_local, group).T, HEAD, axis=1)
    weight = jnp.tile(weight, (slab_rows // group, 1))
    gain = jnp.tile(head_gain, kv_local).reshape(1, -1)
    width = depth // n_tp
    return pl.pallas_call(
        functools.partial(second_kernel, n_kv, n_tp, kv_local, group),
        out_shape=jax.ShapeDtypeStruct((batch, width), BF16),
        in_specs=[vmem] * 6 + [hbm] * 4,
        out_specs=vmem,
        scratch_shapes=[
            pltpu.VMEM(w_out.shape, BF16),
            pltpu.VMEM(second_gate.shape, BF16),
            pltpu.VMEM(second_up.shape, BF16),
            pltpu.VMEM(second_down.shape, BF16),
            pltpu.VMEM((n_kv - 1,) + o_part.shape[1:], BF16),
            pltpu.VMEM((n_kv - 1,) + lse_part.shape[1:], F32),
            pltpu.VMEM(o_part.shape[1:], BF16),
            pltpu.VMEM(o_part.shape, BF16),
            *ffn_buffers,
            *tp_buffers,
            pltpu.VMEM((n_tp, batch, width), BF16),
            pltpu.VMEM((n_tp - 1, batch, width), BF16),
            pltpu.SemaphoreType.DMA((4,)),
            dma_sems(n_kv),
            dma_sems(n_kv),
            dma_sems(n_kv),
            dma_sems(n_kv),
            dma_sems(n_kv),
            dma_sems(n_tp),
            dma_sems(n_tp),
        ],
        compiler_params=params(2),
    )(
        h1, o_part, lse_part, weight, gain, second_gain.reshape(1, -1),
        w_out, second_gate, second_up, second_down,
    )


def solution(mesh):
    placed = (
        P(None, ("kv", "tp")),
        P("kv"),
        P("kv", "tp"),
        P("kv", "tp"),
        P("tp", "kv"),
        P("kv"),
        P("kv", "tp"),
        P(None, "kv", "tp"),
        P(None, "kv", "tp"),
        P("tp"),
        P(),
        P("tp", "kv"),
        P("kv"),
        P("kv", "tp"),
        P("kv", "tp"),
        P("tp", "kv"),
    )
    return jax.shard_map(
        functools.partial(on_device, mesh.shape["kv"], mesh.shape["tp"]),
        mesh=mesh,
        in_specs=placed,
        out_specs=P(None, ("kv", "tp")),
        check_vma=False,
    )
```
